32 devices in a mesh: sp: 16 (over z, y, x), tp: 2 (over core).
Axes of the slice: x: 2, y: 2, z: 4, core: 2. Of those that a mesh axis runs over, the one named last changes fastest.
Arguments:
- input_activity: bfloat16 [8, 1024, 1024], P(None, ('sp', 'tp')), may hold values from -6 to 6
- norm_gain: bfloat16 [1024], replicated, may hold values from 0.75 to 1.25
- w_query: bfloat16 [1024, 256], P(None, 'tp'), may hold values from -0.1875 to 0.1875
- w_key: bfloat16 [1024, 256], P(None, 'tp'), may hold values from -0.1875 to 0.1875
- w_value: bfloat16 [1024, 512], P(None, 'tp'), may hold values from -0.1875 to 0.1875
- w_gate: bfloat16 [1024, 512], P(None, 'tp'), may hold values from -0.1875 to 0.1875
- head_gain: bfloat16 [4, 128], P('tp'), may hold values from 0.75 to 1.25
- w_out: bfloat16 [512, 1024], P('tp'), may hold values from -0.25 to 0.25
- initial_state: float32 [8, 4, 64, 128], P(None, 'tp'), may hold values from -24 to 24
Outputs:
- output: bfloat16 [8, 1024, 1024], P(None, ('sp', 'tp'))
- closing_memory: float32 [8, 4, 64, 128], P(None, 'tp')
The draws below stay inside these ranges and needn't reach their ends.
All inputs are finite; a program needn't handle non-finite values.
Results may differ from the reference program's by a relative error of at most 0.015.
Values may be sent and summed in bfloat16 or wider, within the bound.
A program may use at most 64 MiB of HBM per device.

```python
import jax
import jax.numpy as jnp
from jax import lax

SEQS = 8
STRETCH = 64
D = 1024
HEADS = 4
DK = 64
DV = 128
SEQ = 1024


def shard_levels(stream_key, dims, split, low, high):
    def one(axis_at, parts):
        steps = jax.random.uniform(jax.random.fold_in(jax.random.fold_in(stream_key, 6), axis_at), (parts,), jnp.float32, low / len(split), high / len(split))
        return jnp.repeat(jnp.exp(steps), dims[axis_at] // parts).reshape((-1,) + (1,) * (len(dims) - axis_at - 1))

    level = one(*split[0])
    for cut in split[1:]:
        level = level * one(*cut)
    return level


def normal_values(key, dims, width, most, split=(), kind=jnp.bfloat16):
    result = width * jax.random.normal(key, dims, jnp.float32)
    if split:
        result = result * shard_levels(key, dims, split, -0.22, 0.18)
    return jnp.clip(result, -most, most).astype(kind)


def setup_inputs(seed: int = 0) -> dict:
    key_of = jax.random.split(jax.random.key(seed), 10)
    return {
        "input_activity": normal_values(key_of[0], (SEQS, SEQ, D), 1.0, 6.0, ((1, 32),)),
        "norm_gain": jnp.clip(1.0 + 0.05 * jax.random.normal(key_of[1], (D,), jnp.float32), 0.75, 1.25).astype(jnp.bfloat16),
        "w_query": normal_values(key_of[2], (D, HEADS * DK), D ** -0.5, 0.1875, ((1, 2),)),
        "w_key": normal_values(key_of[3], (D, HEADS * DK), D ** -0.5, 0.1875, ((1, 2),)),
        "w_value": normal_values(key_of[4], (D, HEADS * DV), D ** -0.5, 0.1875, ((1, 2),)),
        "w_gate": normal_values(key_of[5], (D, HEADS * DV), D ** -0.5, 0.1875, ((1, 2),)),
        "head_gain": jnp.clip(1.0 + 0.05 * jax.random.normal(key_of[6], (HEADS, DV), jnp.float32), 0.75, 1.25).astype(jnp.bfloat16),
        "w_out": normal_values(key_of[7], (HEADS * DV, D), (HEADS * DV) ** -0.5, 0.25, ((0, 2),)),
        "initial_state": normal_values(key_of[8], (SEQS, HEADS, DK, DV), (SEQ ** 0.5 / 8), 24.0, ((1, 2),), jnp.float32),
    }


EPS = 1e-06
ROPE_BASE = 10000.0

def rotate(values_in, places):
    size_last = values_in.shape[-1]
    half = size_last // 2
    freqs = ROPE_BASE ** (-jnp.arange(0, size_last, 2, dtype=jnp.float32) / size_last)
    angle = places[:, None] * freqs[None, :]
    cosine = jnp.cos(angle)[None, :, None, :]
    sine = jnp.sin(angle)[None, :, None, :]
    first = values_in[..., :half]
    second = values_in[..., half:]
    return jnp.concatenate([first * cosine - second * sine, first * sine + second * cosine], axis=-1)

def reference(input_activity, norm_gain, w_query, w_key, w_value, w_gate, head_gain, w_out, initial_state):
    floats = input_activity.astype(jnp.float32)
    scaled_unit = (floats * lax.rsqrt(lax.optimization_barrier(jnp.mean(floats * floats, axis=-1, keepdims=True)) + EPS) * norm_gain.astype(jnp.float32)).astype(jnp.bfloat16)
    flat = scaled_unit.reshape(SEQS * SEQ, D)

    def project(weight):
        return jnp.dot(flat, weight, preferred_element_type=jnp.float32).astype(jnp.bfloat16).reshape(SEQS, SEQ, HEADS, -1)
    queries = project(w_query)
    keys_all = project(w_key)
    values_all = project(w_value)
    gates = project(w_gate)
    places = jnp.arange(SEQ, dtype=jnp.float32)
    rot_query = rotate(queries.astype(jnp.float32), places).astype(jnp.bfloat16)
    rot_key = (rotate(keys_all.astype(jnp.float32), places) * DK ** (-0.5)).astype(jnp.bfloat16)
    log_decay = -(0.25 + 0.25 * jnp.arange(HEADS, dtype=jnp.float32)) / SEQ
    blocks = SEQ // STRETCH

    def split_into_groups(field_in):
        return field_in.reshape(SEQS, blocks, STRETCH, HEADS, field_in.shape[-1]).transpose(0, 1, 3, 2, 4).astype(jnp.float32)
    query_blocks = split_into_groups(rot_query)
    key_blocks = split_into_groups(rot_key)
    value_blocks = split_into_groups(values_all)
    steps_idx = jnp.arange(STRETCH, dtype=jnp.float32)
    start_positions = steps_idx[:, None] - steps_idx[None, :]
    mask = jnp.where(start_positions[None] >= 0, jnp.exp(jnp.maximum(start_positions, 0.0)[None] * log_decay[:, None, None]), 0.0)
    scores = jnp.einsum('snhcd,snhkd->snhck', query_blocks, key_blocks) * mask[None, None]
    scores = scores.astype(jnp.bfloat16).astype(jnp.float32)
    inner = jnp.einsum('snhck,snhke->snhce', scores, value_blocks)
    key_decay = jnp.exp((STRETCH - 1 - steps_idx)[None, :] * log_decay[:, None])
    weighted_key = (key_blocks * key_decay[None, None, :, :, None]).astype(jnp.bfloat16).astype(jnp.float32)
    local_state = jnp.einsum('snhcd,snhce->snhde', weighted_key, value_blocks)
    block_decay = jnp.exp(STRETCH * log_decay)[None, :, None, None]

    def advance(state, segment_slice):
        return (state * block_decay + segment_slice, state)
    closing_memory, incoming = lax.scan(advance, initial_state, jnp.moveaxis(local_state, 1, 0))
    query_decay = jnp.exp((steps_idx + 1.0)[None, :] * log_decay[:, None])
    cross = jnp.einsum('snhcd,nshde->snhce', query_blocks * query_decay[None, None, :, :, None], incoming, precision=lax.Precision.HIGHEST)
    retained = (inner + cross).transpose(0, 1, 3, 2, 4).reshape(SEQS, SEQ, HEADS, DV)
    centre = lax.optimization_barrier(jnp.mean(retained, axis=-1, keepdims=True))
    spread = lax.optimization_barrier(jnp.mean(jnp.square(retained - centre), axis=-1, keepdims=True))
    normalized = (retained - centre) * lax.rsqrt(spread + EPS) * head_gain.astype(jnp.float32)[None, None]
    mixed = (jax.nn.silu(gates.astype(jnp.float32)) * normalized).astype(jnp.bfloat16).reshape(SEQS * SEQ, HEADS * DV)
    output = jnp.dot(mixed, w_out, preferred_element_type=jnp.float32).astype(jnp.bfloat16).reshape(SEQS, SEQ, D)
    return (output, closing_memory)
```

```python
import functools
import math

import jax
import jax.numpy as jnp
from jax import lax
from jax.experimental import pallas as pl
from jax.experimental.pallas import tpu as pltpu
from jax.sharding import PartitionSpec as P

EPS = 1e-06
ROPE_BASE = 10000.0
MESH = pl.DeviceIdType.MESH
F32, BF16 = jnp.float32, jnp.bfloat16


def kernel(dims, *refs):
    (n_sp, n_tp, plane, column, heads) = dims
    (x_hbm, gain_hbm, wq_hbm, wk_hbm, wv_hbm, wg_hbm, hgain_hbm, wo_hbm, init_hbm) = refs[:9]
    out_ref, closing_ref = refs[9:11]
    (xbuf, gain, wbuf, hgain, wobuf, initb, nbuf, qm, km, kw, vs, gs, inner, lb, ra, sb, rb, sc, rc, sd, rd,
     mx, mr, lsem, xs, xr, ws, wr, as_, ar, bs, br, cs, cr, ds_, dr, ms, mrs) = refs[11:]
    seqs, half, width = x_hbm.shape
    stretch = half * n_tp
    dk = wq_hbm.shape[1] // heads
    dv = wv_hbm.shape[1] // heads
    kc, vc = heads * dk, heads * dv
    group = (seqs * heads) // plane
    total_len = stretch * n_sp
    rows_half = heads * half
    rows = n_tp * rows_half

    me, t_me = lax.axis_index("sp"), lax.axis_index("tp")
    z_me, p_me = me // plane, me % plane

    barrier = pltpu.get_barrier_semaphore()

    def in_plane(o):
        j = (p_me + o) % plane
        return j, (z_me * plane + j, t_me)

    def in_column(o):
        j = (z_me + o) % column
        return j, (j * plane + p_me, t_me)

    def in_chip(o):
        j = (t_me + o) % n_tp
        return j, (me, j)

    peers = [in_chip(o) for o in range(1, n_tp)]
    peers += [in_plane(o) for o in range(1, plane)]
    peers += [in_column(o) for o in range(1, column)]
    for _, where in peers:
        pl.semaphore_signal(barrier, inc=1, device_id=where, device_id_type=MESH)

    def remote(src, dst, s, r, where):
        return pltpu.make_async_remote_copy(
            src_ref=src, dst_ref=dst, send_sem=s, recv_sem=r, device_id=where, device_id_type=MESH
        )

    loads = [
        (x_hbm, xbuf.at[t_me]),
        (gain_hbm, gain),
        (wq_hbm, wbuf.at[:, 0:kc]),
        (wk_hbm, wbuf.at[:, kc : 2 * kc]),
        (wv_hbm, wbuf.at[:, 2 * kc : 2 * kc + vc]),
        (wg_hbm, wbuf.at[:, 2 * kc + vc :]),
        (hgain_hbm, hgain),
        (init_hbm.at[p_me], initb),
        (wo_hbm, wobuf.at[t_me]),
    ]
    local = [pltpu.make_async_copy(a, b, lsem.at[i]) for i, (a, b) in enumerate(loads)]
    for c in local:
        c.start()

    def fiota(shape, dim):
        return lax.broadcasted_iota(jnp.int32, shape, dim).astype(F32)

    def lg_of(head):
        return (-0.25 / total_len) * (1.0 + (t_me * heads).astype(F32) + head)

    lane = fiota((half, kc), 1)
    lane_head = jnp.floor((lane + 0.5) * (1.0 / dk))
    in_head = lane - dk * lane_head
    upper = jnp.floor((in_head + 0.5) * (2.0 / dk))
    freq = jnp.exp((in_head - upper * (dk // 2)) * (-2.0 * math.log(ROPE_BASE) / dk))
    sign = 2.0 * upper - 1.0
    lane_lg = lg_of(lane_head)
    sub = fiota((half, kc), 0)

    ri, ci = fiota((rows, rows), 0), fiota((rows, rows), 1)

    def places_of(i):
        t = jnp.floor((i + 0.5) * (1.0 / rows_half))
        rest = i - t * rows_half
        h = jnp.floor((rest + 0.5) * (1.0 / half))
        return t * half + rest - h * half, h

    (rpos, rhead), (cpos, chead) = places_of(ri), places_of(ci)
    gap = rpos - cpos
    mask = jnp.where(
        jnp.logical_and(rhead == chead, gap >= 0.0),
        jnp.exp(jnp.maximum(gap, 0.0) * lg_of(rhead)),
        0.0,
    )
    inner_decay = mask

    pl.semaphore_wait(barrier, len(peers))

    sends = []
    for o in range(1, n_tp):
        j, where = in_chip(o)
        sends.append(remote(x_hbm, xbuf.at[t_me], xs.at[j], xr.at[t_me], where))
        sends.append(remote(wo_hbm, wobuf.at[t_me], ws.at[j], wr.at[t_me], where))
    for c in sends:
        c.start()

    for c in local[:6]:
        c.wait()

    def project(t):
        for s in range(seqs):
            xf = xbuf[t, s].astype(F32)
            ms_ = jnp.mean(xf * xf, axis=-1, keepdims=True)
            nbuf[s * half : (s + 1) * half, :] = (
                xf * lax.rsqrt(ms_ + EPS) * gain[...].astype(F32)
            ).astype(BF16)
        pos0 = (t * half).astype(F32)
        angle = (me * stretch).astype(F32) + pos0 + sub
        angle = angle * freq
        cosine, sine = jnp.cos(angle)[None], (jnp.sin(angle) * sign)[None]
        keyd = jnp.exp((stretch - 1.0 - pos0 - sub) * lane_lg)[None]

        def piece(lo, hi):
            y = jnp.dot(nbuf[...], wbuf[:, lo:hi], preferred_element_type=F32)
            return y.astype(BF16)

        qk = piece(0, 2 * kc).astype(F32)

        def turn(v):
            v = v.reshape(seqs, half, kc)
            down = pltpu.roll(v, dk // 2, 2)
            up = pltpu.roll(v, kc - dk // 2, 2)
            return v * cosine + jnp.where(upper[None] > 0.5, down, up) * sine

        rq = turn(qk[:, :kc]).astype(BF16).astype(F32)
        rk = (turn(qk[:, kc:]) * dk**-0.5).astype(BF16).astype(F32)
        wkey = rk * keyd
        v = piece(2 * kc, 2 * kc + vc)
        g = piece(2 * kc + vc, 2 * kc + 2 * vc)
        for h in range(heads):
            keep = jnp.where(lane_head == float(h), 1.0, 0.0)[None]
            at = pl.ds(pl.multiple_of(t * rows_half + h * half, half), half)
            qm[:, at, :] = (rq * keep).astype(BF16)
            km[:, at, :] = (rk * keep).astype(BF16)
            kw[:, at, :] = (wkey * keep).astype(BF16)
            vs[:, at, :] = v[:, h * dv : (h + 1) * dv].reshape(seqs, half, dv)
            gs[:, at, :] = g[:, h * dv : (h + 1) * dv].reshape(seqs, half, dv)

    project(t_me)
    for o in range(1, n_tp):
        j, where = in_chip(o)
        remote(x_hbm, xbuf.at[j], xs.at[j], xr.at[j], where).wait_recv()
        project(j)

    for s in range(seqs):
        state = lax.dot_general(
            kw[s], vs[s], (((0,), (0,)), ((), ())), preferred_element_type=F32
        ).astype(BF16)
        for h in range(heads):
            c = s * heads + h
            lb[c // group, c % group] = state[h * dk : (h + 1) * dk]

    for o in range(1, plane):
        j, where = in_plane(o)
        c = remote(lb.at[j], ra.at[p_me], as_.at[j], ar.at[p_me], where)
        c.start()
        sends.append(c)

    for s in range(seqs):
        scores = lax.dot_general(
            qm[s], km[s], (((1,), (1,)), ((), ())), preferred_element_type=F32
        )
        scores = (scores * inner_decay).astype(BF16)
        inner[s] = jnp.dot(scores, vs[s], preferred_element_type=F32)

    ra[p_me] = lb[p_me]
    for c in local[6:]:
        c.wait()

    group_lg = []
    for g in range(group):
        head = ((p_me * group + g) % heads).astype(F32)
        group_lg.append(lg_of(head) * stretch)

    def power(g, k):
        return jnp.exp(jnp.broadcast_to(group_lg[g] * k, (1, dv)))

    one_block = [power(g, 1.0) for g in range(group)]

    for o in range(1, plane):
        j, where = in_plane(o)
        remote(lb.at[j], ra.at[j], as_.at[j], ar.at[j], where).wait_recv()
    for g in range(group):
        acc = ra[0, g].astype(F32)
        for p in range(1, plane):
            acc = acc * one_block[g] + ra[p, g].astype(F32)
        sb[g] = acc.astype(BF16)
    for o in range(1, column):
        j, where = in_column(o)
        c = remote(sb, rb.at[z_me], bs.at[j], br.at[z_me], where)
        c.start()
        sends.append(c)
    rb[z_me] = sb[...]

    zf = z_me.astype(F32)
    before = [
        [
            power(g, plane * jnp.maximum(zf - 1.0 - z, 0.0)) * jnp.where(z < z_me, 1.0, 0.0)
            for z in range(column)
        ]
        for g in range(group)
    ]
    first = [power(g, plane * zf) for g in range(group)]
    after = [[power(g, float(plane * (column - 1 - z))) for z in range(column)] for g in range(group)]
    whole = [power(g, float(plane * column)) for g in range(group)]

    for o in range(1, column):
        j, where = in_column(o)
        remote(sb, rb.at[j], bs.at[j], br.at[j], where).wait_recv()
    for g in range(group):
        start = initb[g]
        incoming = start * first[g]
        total = start * whole[g]
        for z in range(column):
            a = rb[z, g].astype(F32)
            incoming = incoming + a * before[g][z]
            total = total + a * after[g][z]
        for p in range(plane):
            sc[p, g] = incoming.astype(BF16)
            if p < plane - 1:
                incoming = incoming * one_block[g] + ra[p, g].astype(F32)
        sd[g] = total.astype(BF16)
    for o in range(1, plane):
        j, where = in_plane(o)
        c = remote(sc.at[j], rc.at[p_me], cs.at[j], cr.at[p_me], where)
        c.start()
        sends.append(c)
    for o in range(1, plane):
        j, where = in_plane(o)
        c = remote(sd, rd.at[p_me], ds_.at[j], dr.at[p_me], where)
        c.start()
        sends.append(c)
    rc[p_me] = sc[p_me]
    rd[p_me] = sd[...]

    gain_rows = jnp.concatenate(
        [
            jnp.broadcast_to(hgain[h : h + 1, :].astype(F32), (half, dv))
            for h in range(heads)
        ],
        axis=0,
    )

    for o in range(1, plane):
        j, where = in_plane(o)
        remote(sc.at[j], rc.at[j], cs.at[j], cr.at[j], where).wait_recv()

    def finish(t):
        at = pl.ds(pl.multiple_of(t * rows_half, rows_half), rows_half)
        hpos, hhead = places_of(fiota((rows_half, dv), 0))
        decay = jnp.exp((hpos + (t * half).astype(F32) + 1.0) * lg_of(hhead))
        for s in range(seqs):
            memory = jnp.concatenate(
                [rc[(s * heads + h) // group, (s * heads + h) % group] for h in range(heads)], axis=0
            )
            cross = jnp.dot(qm[s, at, :], memory, preferred_element_type=F32)
            kept = inner[s, at, :] + cross * decay
            centre = jnp.mean(kept, axis=-1, keepdims=True)
            kept = kept - centre
            spread = jnp.mean(kept * kept, axis=-1, keepdims=True)
            gate = gs[s, at, :].astype(F32)
            gate = gate * jax.nn.sigmoid(gate)
            mx[t, s] = (gate * (kept * lax.rsqrt(spread + EPS) * gain_rows)).astype(BF16)

    for o in range(1, n_tp):
        j, where = in_chip(o)
        finish(j)
        c = remote(mx.at[j], mr.at[t_me], ms.at[j], mrs.at[t_me], where)
        c.start()
        sends.append(c)
    finish(t_me)
    mr[t_me] = mx[t_me]

    for o in range(1, plane):
        j, where = in_plane(o)
        remote(sd, rd.at[j], ds_.at[j], dr.at[j], where).wait_recv()
    closing_ref[...] = rd[...].astype(F32)

    for o in range(1, n_tp):
        j, where = in_chip(o)
        remote(wo_hbm, wobuf.at[j], ws.at[j], wr.at[j], where).wait_recv()
        remote(mx.at[j], mr.at[j], ms.at[j], mrs.at[j], where).wait_recv()
    side = jnp.concatenate(
        [
            mr[t, :, h * half : (h + 1) * half, :].reshape(seqs * half, dv)
            for t in range(n_tp)
            for h in range(heads)
        ],
        axis=1,
    )
    weight = wobuf[...].reshape(n_tp * vc, width)
    out_ref[...] = (
        jnp.dot(side, weight, preferred_element_type=F32).astype(BF16).reshape(seqs, half, width)
    )
    for c in sends:
        c.wait_send()


def on_device(n_sp, n_tp, x, gain, wq, wk, wv, wg, hgain, wo, init):
    seqs, half, width = x.shape
    heads, dk, dv = init.shape[1:]
    column = 4 if n_sp % 4 == 0 else 1
    plane = n_sp // column
    group = seqs * heads // plane
    rows = n_tp * heads * half
    kc, vc = heads * dk, heads * dv
    any_spec = pl.BlockSpec(memory_space=pl.ANY)
    vmem_spec = pl.BlockSpec(memory_space=pltpu.VMEM)
    V, D = pltpu.VMEM, pltpu.SemaphoreType.DMA
    state = (group, dk, dv)
    out, closing = pl.pallas_call(
        functools.partial(kernel, (n_sp, n_tp, plane, column, heads)),
        out_shape=(
            jax.ShapeDtypeStruct((seqs, half, width), BF16),
            jax.ShapeDtypeStruct((plane,) + state, F32),
        ),
        in_specs=[any_spec] * 9,
        out_specs=(vmem_spec, vmem_spec),
        scratch_shapes=[
            V((n_tp, seqs, half, width), BF16),
            V((1, width), BF16),
            V((width, 2 * kc + 2 * vc), BF16),
            V((heads, dv), BF16),
            V((n_tp, vc, width), BF16),
            V(state, F32),
            V((seqs * half, width), BF16),
            V((seqs, rows, kc), BF16),
            V((seqs, rows, kc), BF16),
            V((seqs, rows, kc), BF16),
            V((seqs, rows, dv), BF16),
            V((seqs, rows, dv), BF16),
            V((seqs, rows, dv), F32),
            V((plane,) + state, BF16),
            V((plane,) + state, BF16),
            V(state, BF16),
            V((column,) + state, BF16),
            V((plane,) + state, BF16),
            V((plane,) + state, BF16),
            V(state, BF16),
            V((plane,) + state, BF16),
            V((n_tp, seqs, heads * half, dv), BF16),
            V((n_tp, seqs, heads * half, dv), BF16),
            D((9,)),
            D((n_tp,)), D((n_tp,)), D((n_tp,)), D((n_tp,)),
            D((plane,)), D((plane,)),
            D((column,)), D((column,)),
            D((plane,)), D((plane,)),
            D((plane,)), D((plane,)),
            D((n_tp,)), D((n_tp,)),
        ],
        compiler_params=pltpu.CompilerParams(collective_id=0, has_side_effects=True),
    )(x, gain.reshape(1, width), wq, wk, wv, wg, hgain, wo, init.reshape((plane,) + state))
    return out, closing.reshape(init.shape)


def solution(mesh):
    placed = (
        P(None, ("sp", "tp"), None),
        P(),
        P(None, "tp"),
        P(None, "tp"),
        P(None, "tp"),
        P(None, "tp"),
        P("tp", None),
        P("tp", None),
        P(None, "tp", None, None),
    )
    return jax.shard_map(
        functools.partial(on_device, mesh.shape["sp"], mesh.shape["tp"]),
        mesh=mesh,
        in_specs=placed,
        out_specs=(P(None, ("sp", "tp"), None), P(None, "tp", None, None)),
        check_vma=False,
    )
```

```python
import functools
import math

import jax
import jax.numpy as jnp
from jax import lax
from jax.experimental import pallas as pl
from jax.experimental.pallas import tpu as pltpu
from jax.sharding import PartitionSpec as P

EPS = 1e-06
ROPE_BASE = 10000.0
MESH = pl.DeviceIdType.MESH
F32, BF16 = jnp.float32, jnp.bfloat16


def kernel(dims, *refs):
    (n_sp, n_tp, plane, column, heads) = dims
    (x_hbm, gain_ref, wq_hbm, wk_hbm, wv_hbm, wg_hbm, hgain_ref, wo_hbm, init_hbm) = refs[:9]
    out_ref, closing_ref = refs[9:11]
    (xbuf, wbuf, hgain, wobuf, initb, nbuf, qm, km, kw, vs, gs, inner, lb, ra, sb, rb, sc, rc, sd, rd,
     mx, mr, lsem, xs, xr, ws, wr, as_, ar, bs, br, cs, cr, ds_, dr, ms, mrs) = refs[11:]
    seqs, half, width = x_hbm.shape
    stretch = half * n_tp
    dk = wq_hbm.shape[1] // heads
    dv = wv_hbm.shape[1] // heads
    kc, vc = heads * dk, heads * dv
    group = (seqs * heads) // plane
    total_len = stretch * n_sp
    rows_half = heads * half
    rows = n_tp * rows_half

    me, t_me = lax.axis_index("sp"), lax.axis_index("tp")
    z_me, p_me = me // plane, me % plane

    barrier = pltpu.get_barrier_semaphore()

    def in_plane(o):
        j = (p_me + o) % plane
        return j, (z_me * plane + j, t_me)

    def in_column(o):
        j = (z_me + o) % column
        return j, (j * plane + p_me, t_me)

    def in_chip(o):
        j = (t_me + o) % n_tp
        return j, (me, j)

    peers = [in_chip(o) for o in range(1, n_tp)]
    peers += [in_plane(o) for o in range(1, plane)]
    peers += [in_column(o) for o in range(1, column)]
    for _, where in peers:
        pl.semaphore_signal(barrier, inc=1, device_id=where, device_id_type=MESH)

    def remote(src, dst, s, r, where):
        return pltpu.make_async_remote_copy(
            src_ref=src, dst_ref=dst, send_sem=s, recv_sem=r, device_id=where, device_id_type=MESH
        )

    loads = [
        (x_hbm, xbuf.at[t_me]),
        (wq_hbm, wbuf.at[:, 0:kc]),
        (wk_hbm, wbuf.at[:, kc : 2 * kc]),
        (wv_hbm, wbuf.at[:, 2 * kc : 2 * kc + vc]),
        (wg_hbm, wbuf.at[:, 2 * kc + vc :]),
        (hgain_ref, hgain),
        (init_hbm.at[p_me], initb),
        (wo_hbm, wobuf.at[t_me]),
    ]
    local = [pltpu.make_async_copy(a, b, lsem.at[i]) for i, (a, b) in enumerate(loads)]
    for c in local:
        c.start()

    gain = gain_ref[...].reshape(1, width).astype(F32)
    def fiota(shape, dim):
        return lax.broadcasted_iota(jnp.int32, shape, dim).astype(F32)

    def lg_of(head):
        return (-0.25 / total_len) * (1.0 + (t_me * heads).astype(F32) + head)

    lane = fiota((half, kc), 1)
    lane_head = jnp.floor((lane + 0.5) * (1.0 / dk))
    in_head = lane - dk * lane_head
    upper = jnp.floor((in_head + 0.5) * (2.0 / dk))
    freq = jnp.exp((in_head - upper * (dk // 2)) * (-2.0 * math.log(ROPE_BASE) / dk))
    sign = 2.0 * upper - 1.0
    lane_lg = lg_of(lane_head)
    sub = fiota((half, kc), 0)

    ri, ci = fiota((rows, rows), 0), fiota((rows, rows), 1)

    def places_of(i):
        t = jnp.floor((i + 0.5) * (1.0 / rows_half))
        rest = i - t * rows_half
        h = jnp.floor((rest + 0.5) * (1.0 / half))
        return t * half + rest - h * half, h

    (rpos, rhead), (cpos, chead) = places_of(ri), places_of(ci)
    gap = rpos - cpos
    mask = jnp.where(
        jnp.logical_and(rhead == chead, gap >= 0.0),
        jnp.exp(jnp.maximum(gap, 0.0) * lg_of(rhead)),
        0.0,
    )


    local[0].wait()
    with jax.named_scope('w_barrier'):
        pl.semaphore_wait(barrier, len(peers))

    sends = []
    for o in range(1, n_tp):
        j, where = in_chip(o)
        sends.append(remote(xbuf.at[t_me], xbuf.at[t_me], xs.at[j], xr.at[t_me], where))
    for c in sends:
        c.start()

    with jax.named_scope('w_load'):
        for c in local[1:5]:
            c.wait()

    def project(t):
        for s in range(seqs):
            xf = xbuf[t, s].astype(F32)
            ms_ = jnp.mean(xf * xf, axis=-1, keepdims=True)
            nbuf[s * half : (s + 1) * half, :] = (
                xf * lax.rsqrt(ms_ + EPS) * gain
            ).astype(BF16)
        pos0 = (t * half).astype(F32)
        angle = (me * stretch).astype(F32) + pos0 + sub
        angle = angle * freq
        cosine, sine = jnp.cos(angle)[None], (jnp.sin(angle) * sign)[None]
        keyd = jnp.exp((stretch - 1.0 - pos0 - sub) * lane_lg)[None]

        def piece(lo, hi):
            y = jnp.dot(nbuf[...], wbuf[:, lo:hi], preferred_element_type=F32)
            return y.astype(BF16)

        qk = piece(0, 2 * kc).astype(F32)

        def turn(v):
            v = v.reshape(seqs, half, kc)
            down = pltpu.roll(v, dk // 2, 2)
            up = pltpu.roll(v, kc - dk // 2, 2)
            return v * cosine + jnp.where(upper[None] > 0.5, down, up) * sine

        rq = turn(qk[:, :kc]).astype(BF16).astype(F32)
        rk = (turn(qk[:, kc:]) * dk**-0.5).astype(BF16).astype(F32)
        wkey = rk * keyd
        v = piece(2 * kc, 2 * kc + vc)
        g = piece(2 * kc + vc, 2 * kc + 2 * vc)
        for h in range(heads):
            keep = jnp.where(lane_head == float(h), 1.0, 0.0)[None]
            at = pl.ds(pl.multiple_of(t * rows_half + h * half, half), half)
            qm[:, at, :] = (rq * keep).astype(BF16)
            km[:, at, :] = (rk * keep).astype(BF16)
            kw[:, at, :] = (wkey * keep).astype(BF16)
            vs[:, at, :] = v[:, h * dv : (h + 1) * dv].reshape(seqs, half, dv)
            gs[:, at, :] = g[:, h * dv : (h + 1) * dv].reshape(seqs, half, dv)

    with jax.named_scope('project_own'):
        project(t_me)
    for o in range(1, n_tp):
        j, where = in_chip(o)
        with jax.named_scope('w_x'):
            remote(xbuf.at[j], xbuf.at[j], xs.at[j], xr.at[j], where).wait_recv()
        with jax.named_scope('project_other'):
            project(j)

    for s in range(seqs):
        state = lax.dot_general(
            kw[s], vs[s], (((0,), (0,)), ((), ())), preferred_element_type=F32
        ).astype(BF16)
        for h in range(heads):
            c = s * heads + h
            lb[c // group, c % group] = state[h * dk : (h + 1) * dk]

    def to_plane(src, dst, ss, rs, g):
        for o in range(1, plane):
            j, where = in_plane(o)
            c = remote(src(j), dst.at[p_me, g], ss.at[j, g], rs.at[p_me, g], where)
            c.start()
            sends.append(c)

    def from_plane(dst, ss, rs, g):
        for o in range(1, plane):
            j, where = in_plane(o)
            remote(dst.at[j, g], dst.at[j, g], ss.at[j, g], rs.at[j, g], where).wait_recv()

    for g in range(group):
        to_plane(lambda j: lb.at[j, g], ra, as_, ar, g)

    for o in range(1, n_tp):
        j, where = in_chip(o)
        c = remote(wo_hbm, wobuf.at[t_me], ws.at[j], wr.at[t_me], where)
        c.start()
        sends.append(c)

    for s in range(seqs):
        scores = lax.dot_general(
            qm[s], km[s], (((1,), (1,)), ((), ())), preferred_element_type=F32
        )
        scores = (scores * mask).astype(BF16)
        inner[s] = jnp.dot(scores, vs[s], preferred_element_type=F32)

    ra[p_me] = lb[p_me]
    for c in local[5:]:
        c.wait()

    group_lg = []
    for g in range(group):
        head = ((p_me * group + g) % heads).astype(F32)
        group_lg.append(lg_of(head) * stretch)

    def power(g, k):
        return jnp.exp(jnp.broadcast_to(group_lg[g] * k, (1, dv)))

    one_block = [power(g, 1.0) for g in range(group)]

    zf = z_me.astype(F32)
    before = [
        [
            power(g, plane * jnp.maximum(zf - 1.0 - z, 0.0)) * jnp.where(z < z_me, 1.0, 0.0)
            for z in range(column)
        ]
        for g in range(group)
    ]
    first = [power(g, plane * zf) for g in range(group)]
    after = [[power(g, float(plane * (column - 1 - z))) for z in range(column)] for g in range(group)]
    whole = [power(g, float(plane * column)) for g in range(group)]

    for g in range(group):
        with jax.named_scope('w_a'):
            from_plane(ra, as_, ar, g)
        acc = ra[0, g].astype(F32)
        for p in range(1, plane):
            acc = acc * one_block[g] + ra[p, g].astype(F32)
        sb[g] = acc.astype(BF16)
        for o in range(1, column):
            j, where = in_column(o)
            c = remote(sb.at[g], rb.at[z_me, g], bs.at[j, g], br.at[z_me, g], where)
            c.start()
            sends.append(c)
        rb[z_me, g] = sb[g]

    for g in range(group):
        with jax.named_scope('w_b'):
            for o in range(1, column):
                j, where = in_column(o)
                remote(sb.at[g], rb.at[j, g], bs.at[j, g], br.at[j, g], where).wait_recv()
        start = initb[g]
        incoming = start * first[g]
        total = start * whole[g]
        for z in range(column):
            a = rb[z, g].astype(F32)
            incoming = incoming + a * before[g][z]
            total = total + a * after[g][z]
        for p in range(plane):
            sc[p, g] = incoming.astype(BF16)
            if p < plane - 1:
                incoming = incoming * one_block[g] + ra[p, g].astype(F32)
        sd[g] = total.astype(BF16)
        to_plane(lambda j: sc.at[j, g], rc, cs, cr, g)
        to_plane(lambda j: sd.at[g], rd, ds_, dr, g)
        rc[p_me, g] = sc[p_me, g]
        rd[p_me, g] = sd[g]

    gain_rows = jnp.concatenate(
        [
            jnp.broadcast_to(hgain[h : h + 1, :].astype(F32), (half, dv))
            for h in range(heads)
        ],
        axis=0,
    )

    half_pos, half_head = places_of(fiota((rows_half, dv), 0))

    def finish(t, s):
        at = pl.ds(pl.multiple_of(t * rows_half, rows_half), rows_half)
        decay = jnp.exp((half_pos + (t * half).astype(F32) + 1.0) * lg_of(half_head))
        memory = jnp.concatenate(
            [rc[(s * heads + h) // group, (s * heads + h) % group] for h in range(heads)], axis=0
        )
        cross = jnp.dot(qm[s, at, :], memory, preferred_element_type=F32)
        kept = inner[s, at, :] + cross * decay
        centre = jnp.mean(kept, axis=-1, keepdims=True)
        kept = kept - centre
        spread = jnp.mean(kept * kept, axis=-1, keepdims=True)
        gate = gs[s, at, :].astype(F32)
        gate = gate * jax.nn.sigmoid(gate)
        mx[t, s] = (gate * (kept * lax.rsqrt(spread + EPS) * gain_rows)).astype(BF16)

    needs = [max((s * heads + h) % group for h in range(heads)) for s in range(seqs)]
    for g in range(group):
        with jax.named_scope('w_c'):
            from_plane(rc, cs, cr, g)
        ready = [s for s in range(seqs) if needs[s] == g]
        for o in range(1, n_tp):
            j, where = in_chip(o)
            for s in ready:
                finish(j, s)
            if g == group - 1:
                c = remote(mx.at[j], mr.at[t_me], ms.at[j], mrs.at[t_me], where)
                c.start()
                sends.append(c)
        for s in ready:
            finish(t_me, s)
    mr[t_me] = mx[t_me]

    for g in range(group):
        with jax.named_scope('w_d'):
            from_plane(rd, ds_, dr, g)
    closing_ref[...] = rd[...].astype(F32)

    for o in range(1, n_tp):
        j, where = in_chip(o)
        remote(wo_hbm, wobuf.at[j], ws.at[j], wr.at[j], where).wait_recv()
        with jax.named_scope('w_m'):
            remote(mx.at[j], mr.at[j], ms.at[j], mrs.at[j], where).wait_recv()
    side = jnp.concatenate(
        [
            mr[t, :, h * half : (h + 1) * half, :].reshape(seqs * half, dv)
            for t in range(n_tp)
            for h in range(heads)
        ],
        axis=1,
    )
    weight = wobuf[...].reshape(n_tp * vc, width)
    out_ref[...] = (
        jnp.dot(side, weight, preferred_element_type=F32).astype(BF16).reshape(seqs, half, width)
    )
    for c in sends:
        c.wait_send()


def on_device(n_sp, n_tp, x, gain, wq, wk, wv, wg, hgain, wo, init):
    seqs, half, width = x.shape
    heads, dk, dv = init.shape[1:]
    column = 4 if n_sp % 4 == 0 else 1
    plane = n_sp // column
    group = seqs * heads // plane
    rows = n_tp * heads * half
    kc, vc = heads * dk, heads * dv
    any_spec = pl.BlockSpec(memory_space=pl.ANY)
    vmem_spec = pl.BlockSpec(memory_space=pltpu.VMEM)
    V, D = pltpu.VMEM, pltpu.SemaphoreType.DMA
    state = (group, dk, dv)
    out, closing = pl.pallas_call(
        functools.partial(kernel, (n_sp, n_tp, plane, column, heads)),
        out_shape=(
            jax.ShapeDtypeStruct((seqs, half, width), BF16),
            jax.ShapeDtypeStruct((plane,) + state, F32),
        ),
        in_specs=[any_spec, vmem_spec] + [any_spec] * 7,
        out_specs=(vmem_spec, vmem_spec),
        scratch_shapes=[
            V((n_tp, seqs, half, width), BF16),
            V((width, 2 * kc + 2 * vc), BF16),
            V((heads, dv), BF16),
            V((n_tp, vc, width), BF16),
            V(state, F32),
            V((seqs * half, width), BF16),
            V((seqs, rows, kc), BF16),
            V((seqs, rows, kc), BF16),
            V((seqs, rows, kc), BF16),
            V((seqs, rows, dv), BF16),
            V((seqs, rows, dv), BF16),
            V((seqs, rows, dv), F32),
            V((plane,) + state, BF16),
            V((plane,) + state, BF16),
            V(state, BF16),
            V((column,) + state, BF16),
            V((plane,) + state, BF16),
            V((plane,) + state, BF16),
            V(state, BF16),
            V((plane,) + state, BF16),
            V((n_tp, seqs, heads * half, dv), BF16),
            V((n_tp, seqs, heads * half, dv), BF16),
            D((8,)),
            D((n_tp,)), D((n_tp,)), D((n_tp,)), D((n_tp,)),
            D((plane, group)), D((plane, group)),
            D((column, group)), D((column, group)),
            D((plane, group)), D((plane, group)),
            D((plane, group)), D((plane, group)),
            D((n_tp,)), D((n_tp,)),
        ],
        compiler_params=pltpu.CompilerParams(collective_id=0, has_side_effects=True),
    )(x, gain, wq, wk, wv, wg, hgain, wo, init.reshape((plane,) + state))
    return out, closing.reshape(init.shape)


def solution(mesh):
    placed = (
        P(None, ("sp", "tp"), None),
        P(),
        P(None, "tp"),
        P(None, "tp"),
        P(None, "tp"),
        P(None, "tp"),
        P("tp", None),
        P("tp", None),
        P(None, "tp", None, None),
    )
    return jax.shard_map(
        functools.partial(on_device, mesh.shape["sp"], mesh.shape["tp"]),
        mesh=mesh,
        in_specs=placed,
        out_specs=(P(None, ("sp", "tp"), None), P(None, "tp", None, None)),
        check_vma=False,
    )
```
